256 devices in a mesh: ra: 16 (over y, x), cb: 16 (over z, core).
Axes of the slice: x: 4, y: 4, z: 8, core: 2. Of those that a mesh axis runs over, the one named last changes fastest.
Arguments:
- hidden_states: bfloat16 [384, 4096], P(None, 'ra'), may hold values from -40 to 40
- gain_first: bfloat16 [4096], P('ra'), may hold values from 0.099609375 to 1.8984375
- gate_first: bfloat16 [4096, 11264], P('ra', 'cb'), may hold values from -0.09375 to 0.09375
- up_first: bfloat16 [4096, 11264], P('ra', 'cb'), may hold values from -0.09375 to 0.09375
- down_first: bfloat16 [11264, 4096], P('cb', 'ra'), may hold values from -0.0546875 to 0.0546875
- gain_second: bfloat16 [4096], P('ra'), may hold values from 0.099609375 to 1.8984375
- gate_second: bfloat16 [4096, 11264], P('ra', 'cb'), may hold values from -0.09375 to 0.09375
- up_second: bfloat16 [4096, 11264], P('ra', 'cb'), may hold values from -0.09375 to 0.09375
- down_second: bfloat16 [11264, 4096], P('cb', 'ra'), may hold values from -0.0546875 to 0.0546875
- gain_last: bfloat16 [4096], P('ra'), may hold values from 0.099609375 to 1.8984375
Outputs:
- closed: bfloat16 [384, 4096], P(None, 'ra')
The draws below stay inside these ranges and needn't reach their ends.
All inputs are finite; a program needn't handle non-finite values.
Results may differ from the reference program's by a relative error of at most 0.0098.
Values may be sent and summed in bfloat16 or wider, within the bound.
A program may use at most 64 MiB of HBM per device.

```python
import math
import jax
import jax.numpy as jnp
from jax import lax

D = 4096
FF = 11264
TOKENS = 384


def draw_hidden_states(key, part):
    key_base, key_row, key_col = jax.random.split(key, 3)
    position = jnp.arange(D, dtype=jnp.float32) / D
    rough = jnp.exp(jax.random.uniform(key_col, (D,), jnp.float32, -0.35, 0.35))
    col_scale = 0.5 * jnp.exp(math.log(4.0) * position) * rough
    base = jnp.clip(jax.random.normal(key_base, (TOKENS, D), jnp.float32), -4.0, 4.0)
    row_scale = jnp.exp(jax.random.uniform(key_row, (TOKENS, 1), jnp.float32, math.log(0.3), math.log(3.0)))
    return (base * row_scale * col_scale[None, :]).astype(jnp.bfloat16)


def block_levels(own_key, dims, shards, low, top_value):
    loudness, own = 1.0, jax.random.fold_in(own_key, 6)
    for dim, blocks in shards:
        steps = jnp.exp(jax.random.uniform(jax.random.fold_in(own, dim), (blocks,), jnp.float32, low / len(shards), top_value / len(shards)))
        loudness = loudness * jnp.repeat(steps, dims[dim] // blocks).reshape([-1 if axis == dim else 1 for axis in range(len(dims))])
    return loudness


def centred(own_key, dims, spread, limit, shards=(), kind=jnp.bfloat16):
    result = jax.random.normal(own_key, dims, jnp.float32) * spread
    if len(shards) > 0:
        result = block_levels(own_key, dims, shards, -0.22, 0.18) * result
    return jnp.clip(result, min=-limit, max=limit).astype(kind)


def setup_inputs(seed: int = 0) -> dict:
    keys = jax.random.split(jax.random.key(seed), 11)
    hidden_states = draw_hidden_states(jax.random.fold_in(keys[10], 71), 0)
    gain_first = jnp.clip(1.0 + 0.18 * jax.random.normal(keys[1], (D,), jnp.float32), 0.099609375, 1.8984375).astype(jnp.bfloat16)
    gate_first = centred(keys[2], (D, FF), D ** -0.5, 0.09375, ((0, 16), (1, 16)))
    up_first = centred(keys[3], (D, FF), D ** -0.5, 0.09375, ((0, 16), (1, 16)))
    down_first = centred(keys[4], (FF, D), FF ** -0.5, 0.0546875, ((0, 16), (1, 16)))
    gain_second = jnp.clip(1.0 + 0.18 * jax.random.normal(keys[5], (D,), jnp.float32), 0.099609375, 1.8984375).astype(jnp.bfloat16)
    gate_second = centred(keys[6], (D, FF), D ** -0.5, 0.09375, ((0, 16), (1, 16)))
    up_second = centred(keys[7], (D, FF), D ** -0.5, 0.09375, ((0, 16), (1, 16)))
    down_second = centred(keys[8], (FF, D), FF ** -0.5, 0.0546875, ((0, 16), (1, 16)))
    gain_last = jnp.clip(1.0 + 0.18 * jax.random.normal(keys[9], (D,), jnp.float32), 0.099609375, 1.8984375).astype(jnp.bfloat16)
    return {"hidden_states": hidden_states, "gain_first": gain_first, "gate_first": gate_first, "up_first": up_first, "down_first": down_first, "gain_second": gain_second, "gate_second": gate_second, "up_second": up_second, "down_second": down_second, "gain_last": gain_last}


norm_eps = 1e-06
residual_weight = 0.25
branch_weight = 0.5

def half_step(stream, gain, w_gate, w_up, w_down):
    values = stream.astype(jnp.float32)
    scale = lax.rsqrt(lax.optimization_barrier(jnp.mean(values * values, axis=1, keepdims=True)) + norm_eps)
    normed = (values * gain.astype(jnp.float32)).astype(jnp.bfloat16)
    gate = jnp.dot(normed, w_gate, preferred_element_type=jnp.float32) * scale
    upper = jnp.dot(normed, w_up, preferred_element_type=jnp.float32) * scale
    hidden = (jax.nn.silu(gate) * upper).astype(jnp.bfloat16)
    branch = jnp.dot(hidden, w_down, preferred_element_type=jnp.float32)
    return (residual_weight * values + branch_weight * branch).astype(jnp.bfloat16)

def reference(hidden_states, gain_first, gate_first, up_first, down_first, gain_second, gate_second, up_second, down_second, gain_last):
    first = half_step(hidden_states, gain_first, gate_first, up_first, down_first)
    second = half_step(first, gain_second, gate_second, up_second, down_second)
    values = second.astype(jnp.float32)
    scale = lax.rsqrt(lax.optimization_barrier(jnp.mean(values * values, axis=1, keepdims=True)) + norm_eps)
    return (values * scale * gain_last.astype(jnp.float32)).astype(jnp.bfloat16)
```

```python
import functools

import jax
import jax.numpy as jnp
from jax import lax
from jax.experimental import pallas as pl
from jax.experimental.pallas import tpu as pltpu
from jax.sharding import PartitionSpec as P

MESH = pl.DeviceIdType.MESH
F32, BF16 = jnp.float32, jnp.bfloat16

D = 4096
NORM_EPS = 1e-06
RESIDUAL_WEIGHT = 0.25
BRANCH_WEIGHT = 0.5

N = 16
CHUNKS = 3
PAD = 64


def kernel(
    x_hbm, g1, g2, g3, wg1, wu1, wd1, wg2, wu2, wd2, out,
    x, gain1, gain2, gain3, wg, wu, wd, part, part_in, hid, down, down_in, own, first, sq, sq_in,
    load_sem, send_sem, recv_sem,
):
    ra, cb = lax.axis_index("ra"), lax.axis_index("cb")
    rows, width = x.shape[1:]
    units = wg.shape[1]
    half = units + PAD
    tokens = N * rows

    loads = [
        pltpu.make_async_copy(src, dst, load_sem.at[i])
        for i, (src, dst) in enumerate([
            (x_hbm, x), (g1, gain1), (wg1, wg.at[0]), (wu1, wu.at[0]), (wd1, wd.at[0]),
            (g2, gain2), (wg2, wg.at[1]), (wu2, wu.at[1]), (wd2, wd.at[1]), (g3, gain3),
        ])
    ]
    for load in loads:
        load.start()

    def ra_peer(k):
        return {"ra": lax.rem(ra + k, N)}

    def cb_peer(k):
        return {"cb": lax.rem(cb + k, N)}

    barrier = pltpu.get_barrier_semaphore()
    for k in range(1, N):
        pl.semaphore_signal(barrier, inc=1, device_id=ra_peer(k), device_id_type=MESH)
        pl.semaphore_signal(barrier, inc=1, device_id=cb_peer(k), device_id_type=MESH)

    sent = []

    def send(peer, source, target, block, slot):
        index = len(sent)
        for k in range(1, N):
            pltpu.make_async_remote_copy(
                src_ref=source(k), dst_ref=target(k),
                send_sem=send_sem.at[index], recv_sem=recv_sem.at[index],
                device_id=peer(k), device_id_type=MESH,
            ).start()
        every = pltpu.make_async_remote_copy(
            src_ref=block, dst_ref=block,
            send_sem=send_sem.at[index], recv_sem=recv_sem.at[index],
            device_id=peer(1), device_id_type=MESH,
        )
        sent.append(every)
        return every.wait_recv

    def project(b, c, values, gain):
        squares = jnp.sum(values * values, axis=2, keepdims=True)
        normed = (values * gain[...].astype(F32).reshape(1, 1, width)).reshape(tokens, width).astype(BF16)
        for at, w in ((0, wg), (half, wu)):
            product = lax.dot_general(normed, w[b], (((1,), (1,)), ((), ())), preferred_element_type=F32)
            part[b, c, :, :, at : at + units] = product.reshape(N, rows, units).astype(BF16)
        high = squares.astype(BF16)
        low = (squares - high.astype(F32)).astype(BF16)
        part[b, c, :, :, units:half] = jnp.broadcast_to(high, (N, rows, PAD))
        part[b, c, :, :, half + units :] = jnp.broadcast_to(low, (N, rows, PAD))

    def send_parts(b, c):
        return send(
            ra_peer, lambda k: part.at[b, c, lax.rem(ra + k, N)], lambda k: part_in.at[b, c, k - 1],
            part_in.at[b, c], None,
        )

    def gate(b, c):
        total = part[b, c, ra].astype(F32)
        for k in range(N - 1):
            total += part_in[b, c, k].astype(F32)
        squares = total[:, units : units + 1] + total[:, half + units : half + units + 1]
        scale = lax.rsqrt(squares / D + NORM_EPS)
        g, u = total[:, :units] * scale, total[:, half : half + units] * scale
        hid[b, c, ra] = (g / (1.0 + jnp.exp(-g)) * u).astype(BF16)
        return send(
            ra_peer, lambda k: hid.at[b, c, ra], lambda k: hid.at[b, c, ra],
            hid.at[b, c, pl.ds(0, N - 1)], None,
        )

    def branch(b, c):
        rows_of_all = hid[b, c].astype(F32).reshape(tokens, units).astype(BF16)
        product = jnp.dot(rows_of_all, wd[b], preferred_element_type=F32)
        down[b, c] = product.reshape(N, rows, width).astype(BF16)
        return send(
            cb_peer, lambda k: down.at[b, c, lax.rem(cb + k, N)], lambda k: down_in.at[b, c, k - 1],
            down_in.at[b, c], None,
        )

    def updated(b, c, values):
        total = down[b, c, cb].astype(F32)
        for k in range(N - 1):
            total += down_in[b, c, k].astype(F32)
        return (RESIDUAL_WEIGHT * values.astype(F32) + BRANCH_WEIGHT * total).astype(BF16)

    chunks = range(CHUNKS)
    for load in loads[:4]:
        load.wait()
    waits = [None] * CHUNKS
    for c in chunks:
        project(0, c, x[pl.ds(c * N, N)].astype(F32), gain1)
        if c == 0:
            pl.semaphore_wait(barrier, 2 * (N - 1))
        waits[c] = send_parts(0, c)
    for c in chunks:
        waits[c]()
        waits[c] = gate(0, c)
    loads[4].wait()
    for c in chunks:
        waits[c]()
        waits[c] = branch(0, c)
    for c in chunks:
        waits[c]()
        first[c, cb] = updated(0, c, x[c * N + cb])
        waits[c] = send(
            cb_peer, lambda k: first.at[c, cb], lambda k: first.at[c, cb], first.at[c, pl.ds(0, N - 1)], None
        )
    for load in loads[5:8]:
        load.wait()
    for c in chunks:
        waits[c]()
        project(1, c, first[c].astype(F32), gain2)
        waits[c] = send_parts(1, c)
    for c in chunks:
        waits[c]()
        waits[c] = gate(1, c)
    for load in loads[8:]:
        load.wait()
    for c in chunks:
        waits[c]()
        waits[c] = branch(1, c)
    for c in chunks:
        waits[c]()
        second = updated(1, c, first[c, cb])
        own[c] = second
        values = second.astype(F32)
        sq[c] = jnp.broadcast_to(jnp.sum(values * values, axis=1, keepdims=True), sq.shape[1:])
        waits[c] = send(ra_peer, lambda k: sq.at[c], lambda k: sq_in.at[c, k - 1], sq_in.at[c], None)
    for c in chunks:
        waits[c]()
        squares = sq[c]
        for k in range(N - 1):
            squares += sq_in[c, k]
        scale = lax.rsqrt(squares[:, :1] / D + NORM_EPS)
        out[c * N + cb] = (own[c].astype(F32) * scale * gain3[...].astype(F32).reshape(1, width)).astype(BF16)
        waits[c] = send(
            cb_peer, lambda k: out.at[c * N + cb], lambda k: out.at[c * N + cb], out.at[pl.ds(0, N - 1)], None
        )
    for c in chunks:
        waits[c]()
    for every in sent:
        every.wait_send()


def body(
    hidden_states,
    gain_first,
    gate_first,
    up_first,
    down_first,
    gain_second,
    gate_second,
    up_second,
    down_second,
    gain_last,
):
    tokens, width = hidden_states.shape
    units = gate_first.shape[1]
    rows = tokens // (CHUNKS * N)
    x = hidden_states.reshape(CHUNKS * N, rows, width)
    gains = (gain_first, gain_second, gain_last)
    anywhere, vmem = pl.BlockSpec(memory_space=pltpu.HBM), pl.BlockSpec(memory_space=pltpu.VMEM)
    columns = 2 * (units + PAD)
    out = pl.pallas_call(
        kernel,
        out_shape=jax.ShapeDtypeStruct(x.shape, BF16),
        in_specs=[anywhere] * 10,
        out_specs=vmem,
        scratch_shapes=[
            pltpu.VMEM(x.shape, BF16),
            *[pltpu.VMEM((width,), BF16)] * 3,
            pltpu.VMEM((2, units, width), BF16),
            pltpu.VMEM((2, units, width), BF16),
            pltpu.VMEM((2, units, width), BF16),
            pltpu.VMEM((2, CHUNKS, N, rows, columns), BF16),
            pltpu.VMEM((2, CHUNKS, N - 1, rows, columns), BF16),
            pltpu.VMEM((2, CHUNKS, N, rows, units), BF16),
            pltpu.VMEM((2, CHUNKS, N, rows, width), BF16),
            pltpu.VMEM((2, CHUNKS, N - 1, rows, width), BF16),
            pltpu.VMEM((CHUNKS, rows, width), BF16),
            pltpu.VMEM((CHUNKS, N, rows, width), BF16),
            pltpu.VMEM((CHUNKS, rows, 128), F32),
            pltpu.VMEM((CHUNKS, N - 1, rows, 128), F32),
            pltpu.SemaphoreType.DMA((10,)),
            pltpu.SemaphoreType.DMA((10 * CHUNKS,)),
            pltpu.SemaphoreType.DMA((10 * CHUNKS,)),
        ],
        compiler_params=pltpu.CompilerParams(
            collective_id=0, has_side_effects=True, vmem_limit_bytes=67_043_328
        ),
        name="pair",
    )(x, *gains, gate_first.T, up_first.T, down_first, gate_second.T, up_second.T, down_second)
    return out.reshape(tokens, width)


def solution(mesh):
    return jax.shard_map(
        body,
        mesh=mesh,
        in_specs=(
            P(None, "ra"),
            P("ra"),
            P("ra", "cb"),
            P("ra", "cb"),
            P("cb", "ra"),
            P("ra"),
            P("ra", "cb"),
            P("ra", "cb"),
            P("cb", "ra"),
            P("ra"),
        ),
        out_specs=P(None, "ra"),
        check_vma=False,
    )
```
